256 devices in a mesh: grp: 2 (over y), ep: 64 (over z, x), tp: 2 (over core).
Axes of the slice: x: 4, y: 2, z: 16, core: 2. Of those that a mesh axis runs over, the one named last changes fastest.
The devices are a block of a 4x16x16 slice.
Arguments:
- tokens: bfloat16 [32768, 2048], P(('grp', 'ep', 'tp')), parts along dimension 0, may hold values from -6 to 6
- expert_ids: int32 [32768, 4], P(('grp', 'ep', 'tp')), parts along dimension 0, may hold values from 0 to 127, all different within a row; in each aligned block of 128 rows (0 to 127, 128 to 255, ...) at most 6 rows name the same one
- gate_weights: float32 [32768, 4], P(('grp', 'ep', 'tp')), parts along dimension 0, may hold values from 0.1 to 1
- norm_gain: float32 [2048], replicated, may hold values from 0.1 to 1.9
- expert_gate: bfloat16 [128, 2048, 512], P(('ep', 'tp')), may hold values from -0.125 to 0.125
- expert_up: bfloat16 [128, 2048, 512], P(('ep', 'tp')), may hold values from -0.125 to 0.125
- expert_down: bfloat16 [128, 512, 2048], P(('ep', 'tp'))
- shared_gate: bfloat16 [2048, 512], P(None, 'tp'), may hold values from -0.125 to 0.125
- shared_up: bfloat16 [2048, 512], P(None, 'tp'), may hold values from -0.125 to 0.125
- shared_down: bfloat16 [512, 2048], P('tp')
- out_gain: float32 [2048], replicated, may hold values from 0.1 to 1.9
Outputs:
- layer_out: bfloat16 [32768, 2048], P(('grp', 'ep'), 'tp'), parts along dimension 0
The draws below stay inside these ranges and needn't reach their ends.
There are 2 independent parts, one for each index of `grp`. The reference program is written for one: setup_inputs(seed, part) draws one part's arguments, and reference() takes and returns one part's arrays. A program takes and returns all parts, laid end to end along the dimension named above; an argument that names none is the same for every part. Nothing has to cross between parts.
Inputs may be any that keep to these rules, and one draw needn't show every extreme that they name: `expert_ids`: each row names 4 different experts. Among the 128 rows of one device (aligned blocks of rows), no expert is named more than 6 times, and in every draw some expert is named exactly 6 times by some device.
All inputs are finite; a program needn't handle non-finite values.
Results may differ from the reference program's by a relative error of at most 0.0085.
Values may be sent and summed in bfloat16 or wider, within the bound.
No kernel may reach another device: no remote copies, remote signals or barrier semaphores. Data moves between devices by JAX's collectives and lax.ppermute only.
A program may use at most 64 MiB of HBM per device.

```python
import math
import jax
import jax.numpy as jnp
import numpy as np
from jax import lax

D = 2048
FF = 512
SH = 512
TOPK = 4
TOK_DEV = 128
EXPERTS = 128
CAP = 6
TOKENS = 16384
N_EP = 64
N_TP = 2


def rising_columns(key, shape, fan_in):
    base = jax.random.normal(key, shape, jnp.float32)
    columns = shape[-1]
    rise = 10.0 ** (jnp.arange(columns, dtype=jnp.float32) / (columns - 1))
    return base * rise * fan_in ** (-0.5)


def draw_expert_down(key, part):
    return rising_columns(jax.random.fold_in(key, 11), (EXPERTS, FF, D), FF).astype(jnp.bfloat16)


def draw_shared_down(key, part):
    return rising_columns(jax.random.fold_in(key, 23), (SH, D), SH).astype(jnp.bfloat16)


def block_scale(rng, shape, pieces, least, top_value):
    def one(position, shards_of):
        steps = jax.random.uniform(jax.random.fold_in(jax.random.fold_in(rng, 6), position), (shards_of,), jnp.float32, least / len(pieces), top_value / len(pieces))
        return jnp.repeat(jnp.exp(steps), shape[position] // shards_of).reshape((-1,) + (1,) * (len(shape) - position - 1))

    loudness = one(*pieces[0])
    for cut in pieces[1:]:
        loudness = loudness * one(*cut)
    return loudness


def deal_out(rng, own, number, rows, amount, top, most, skew):
    sequence = jax.random.permutation(rng, amount)
    packed, usual = shares(amount, rows * top, most, skew, True), shares(amount, rows * top, most, skew, False)
    places = jnp.arange(amount)

    def named(tallies, offset_by):
        used = int((tallies > 0).sum())
        fixed = max(1, used // 4)
        moved = fixed + (places - fixed + offset_by * (used - fixed)) % max(1, amount - fixed)
        return jnp.zeros((amount,), jnp.int32).at[sequence[jnp.where(places < fixed, places, moved)]].set(jnp.asarray(tallies, jnp.int32))

    tallies = jnp.where(number % 4 == 0, named(packed, number // 4), named(usual, number - number // 4 - 1))
    mixed = jax.random.permutation(jax.random.fold_in(own, 3), amount)
    donor, sink = mixed[0:amount // 2 * 2:2], mixed[1:amount // 2 * 2:2]
    room = jnp.minimum(tallies[donor] - 1, most - tallies[sink]) // 2
    room = jnp.where((donor == sequence[0]) | (sink == sequence[0]) | (tallies[sink] == 0), 0, jnp.maximum(room, 0))
    moved = jax.random.randint(jax.random.fold_in(own, 4), (amount // 2,), 0, 1 << 20) % (room + 1)
    tallies = tallies.at[donor].add(-moved).at[sink].add(moved)
    labels = jnp.searchsorted(jnp.cumsum(tallies), jnp.arange(rows * top), side="right").astype(jnp.int32)
    table = labels.reshape(top, rows).T
    table = table[jax.random.permutation(jax.random.fold_in(own, 1), rows)]
    offset_by = jax.random.randint(jax.random.fold_in(own, 2), (rows, 1), 0, top)
    return jnp.take_along_axis(table, (jnp.arange(top)[None, :] + offset_by) % top, axis=1)


def shares(amount, total, reach, lean, full):
    loads = [(1 << 20) // math.isqrt(standing ** lean) + 1 for standing in range(1, amount + 1)]
    largest = reach if full else min(reach, max(-(-total // amount), total * loads[0] // sum(loads)))
    least = 1 if total - largest >= amount - 1 else 0
    given, spare = [largest] + [least] * (amount - 1), total - largest - least * (amount - 1)
    while spare > 0:
        movable = [i for i in range(1, amount) if given[i] < largest] or [i for i in range(1, amount) if given[i] < reach]
        whole, remaining = sum([loads[i] for i in movable]), spare
        for i in movable:
            extra = min(reach - given[i], max(1, remaining * loads[i] // whole), spare)
            given[i] = given[i] + extra
            spare = spare - extra
    return np.array(given)


def normal_values(rng, dims, deviation, bound, pieces=(), kind=jnp.bfloat16):
    drawn = deviation * jax.random.normal(rng, dims, jnp.float32)
    if pieces:
        drawn = drawn * block_scale(rng, dims, pieces, -0.22, 0.18)
    return jnp.clip(drawn, -bound, bound).astype(kind)


def setup_inputs(seed: int = 0, part: int = 0) -> dict:
    arg_keys = jax.random.split(jax.random.key(seed), 12)
    part_keys = jax.random.split(jax.random.fold_in(arg_keys[11], part), 12)
    tokens = normal_values(part_keys[0], (TOKENS, D), 1.0, 6.0, ((0, 128),))
    expert_ids_keys = jax.random.split(jax.random.fold_in(part_keys[1], 1), TOKENS // TOK_DEV)
    expert_ids_turns = jax.random.permutation(jax.random.fold_in(part_keys[1], 3), TOKENS // TOK_DEV)
    expert_ids = jax.vmap(lambda own, number: deal_out(jax.random.fold_in(part_keys[1], 2), own, number, TOK_DEV, EXPERTS, TOPK, CAP, 2))(expert_ids_keys, expert_ids_turns).reshape((TOKENS, TOPK))
    gate_weights = jnp.clip(jnp.exp(math.log(1.0) - 2.3025851 * jax.random.uniform(part_keys[2], (TOKENS, TOPK), jnp.float32) ** block_scale(part_keys[2], (TOKENS, TOPK), ((0, 128),), -0.2, 0.2)), 0.1, 1.0)
    norm_gain = jnp.clip(1.0 + 0.18 * jax.random.normal(arg_keys[3], (D,), jnp.float32), 0.1, 1.9)
    expert_gate = normal_values(arg_keys[4], (EXPERTS, D, FF), D ** -0.5, 0.125, ((0, 128),))
    expert_up = normal_values(arg_keys[5], (EXPERTS, D, FF), D ** -0.5, 0.125, ((0, 128),))
    expert_down = draw_expert_down(jax.random.fold_in(arg_keys[11], 71), part)
    shared_gate = normal_values(arg_keys[7], (D, SH), D ** -0.5, 0.125, ((1, 2),))
    shared_up = normal_values(arg_keys[8], (D, SH), D ** -0.5, 0.125, ((1, 2),))
    shared_down = draw_shared_down(jax.random.fold_in(arg_keys[11], 71), part)
    out_gain = jnp.clip(1.0 + 0.18 * jax.random.normal(arg_keys[10], (D,), jnp.float32), 0.1, 1.9)
    return {"tokens": tokens, "expert_ids": expert_ids, "gate_weights": gate_weights, "norm_gain": norm_gain, "expert_gate": expert_gate, "expert_up": expert_up, "expert_down": expert_down, "shared_gate": shared_gate, "shared_up": shared_up, "shared_down": shared_down, "out_gain": out_gain}


def reference(tokens, expert_ids, gate_weights, norm_gain, expert_gate, expert_up, expert_down, shared_gate, shared_up, shared_down, out_gain):
    values = tokens.astype(jnp.float32)
    scale = lax.rsqrt(lax.optimization_barrier(jnp.mean(values * values, axis=1, keepdims=True)) + 1e-06)
    normed = (values * scale * norm_gain).astype(jnp.bfloat16)
    flat_ids = expert_ids.reshape(-1)
    flat_gates = gate_weights.reshape(-1)
    copy_count = TOKENS * TOPK
    most_rows = N_EP * N_TP * CAP

    def one_expert(total, inputs):
        w_gate, w_up, w_down, expert_index = inputs
        positions = jnp.nonzero(flat_ids == expert_index, size=most_rows, fill_value=copy_count)[0].astype(jnp.int32)
        valid = positions < copy_count
        clipped = jnp.minimum(positions, copy_count - 1)
        token_index = clipped // TOPK
        weight = jnp.where(valid, flat_gates[clipped], 0.0)
        rows = normed[token_index]
        gate = jnp.dot(rows, w_gate, preferred_element_type=jnp.float32)
        upper = jnp.dot(rows, w_up, preferred_element_type=jnp.float32)
        hidden = (jax.nn.silu(gate) * upper).astype(jnp.bfloat16)
        result = jnp.dot(hidden, w_down, preferred_element_type=jnp.float32).astype(jnp.bfloat16)
        total = total.at[token_index].add(result.astype(jnp.float32) * weight[:, None])
        return (total, None)
    routed, _ = lax.scan(one_expert, jnp.zeros((TOKENS, D), jnp.float32), (expert_gate, expert_up, expert_down, jnp.arange(EXPERTS, dtype=jnp.int32)))
    shared_hidden = (jax.nn.silu(jnp.dot(normed, shared_gate, preferred_element_type=jnp.float32)) * jnp.dot(normed, shared_up, preferred_element_type=jnp.float32)).astype(jnp.bfloat16)
    shared_out = jnp.dot(shared_hidden, shared_down, preferred_element_type=jnp.float32)
    mixed = (routed + shared_out).astype(jnp.bfloat16).astype(jnp.float32)
    final_scale = lax.rsqrt(lax.optimization_barrier(jnp.mean(mixed * mixed, axis=1, keepdims=True)) + 1e-06)
    return (mixed * final_scale * out_gain).astype(jnp.bfloat16)
```

```python
import functools

import jax
import jax.numpy as jnp
from jax import lax
from jax.experimental import pallas as pl
from jax.experimental.pallas import tpu as pltpu
from jax.sharding import PartitionSpec as P


TOPK = 4
ROW = 4
F32 = jnp.float32
BF16 = jnp.bfloat16
VMEM = pl.BlockSpec(memory_space=pltpu.VMEM)
OWN, OTHER = "own", "other"
BATCHES = (
    ((OWN, 0), (OWN, 1), (OTHER, 1), (OWN, 2), (OTHER, 2), (OWN, 3), (OTHER, 3), (OWN, 4)),
    ((OTHER, 4), (OWN, 5), (OTHER, 5), (OWN, 6)),
    ((OTHER, 6), (OWN, 7), (OTHER, 7), (OWN, 8)),
)
DENSE = {OWN: 6, OTHER: 5}


def iota(shape, dim):
    return lax.broadcasted_iota(jnp.int32, shape, dim)


def call(body, outs, *args, flops=0, limit=12):
    moved = sum(a.size * a.dtype.itemsize for a in (*args, *outs))
    return pl.pallas_call(
        body,
        out_shape=tuple(outs),
        in_specs=[VMEM] * len(args),
        out_specs=tuple(VMEM for _ in outs),
        compiler_params=pltpu.CompilerParams(vmem_limit_bytes=limit << 20),
        cost_estimate=pl.CostEstimate(flops=flops, bytes_accessed=moved, transcendentals=0),
    )(*args)


def place():
    ep = lax.axis_index("ep")
    return ep // ROW, ep % ROW, lax.axis_index("tp")


def normalized(values, gain):
    scale = lax.rsqrt(jnp.mean(values * values, axis=1, keepdims=True) + 1e-06)
    return (values * scale * gain).astype(BF16)


def silu(v):
    return v / (1.0 + jnp.exp(-v))


def meta_body(experts, ids_ref, gates_ref, out_ref):
    tokens = ids_ref.shape[1]
    ids = ids_ref[...]
    named = [(iota((experts, tokens), 0) == ids[k : k + 1]).astype(F32) for k in range(TOPK)]
    before = (iota((tokens, tokens), 0) < iota((tokens, tokens), 1)).astype(BF16)
    count = jnp.dot(sum(named).astype(BF16), before, preferred_element_type=F32)
    out_ref[0] = ids.astype(F32)
    for k in range(TOPK):
        out_ref[1, k : k + 1] = jnp.sum(named[k] * count, axis=0, keepdims=True)
    out_ref[2] = gates_ref[...]
    out_ref[3] = jnp.zeros_like(gates_ref)


def piece_of(local, x, c):
    shift = ((local >> 1) - x) & (ROW - 1)
    return shift * 2 + ((local & 1) ^ c)


def dense_rows(meta, b, capacity, rows):
    z, x, c = place()
    expert = meta[0].astype(jnp.int32)
    slot = meta[1].astype(jnp.int32)
    row = piece_of(expert & (2 * ROW - 1), x, c) * rows + b * capacity + slot
    return jnp.where((expert // (2 * ROW)) == z, row, -1)


def far_rows(meta, planes, capacity):
    z, _, c = place()
    expert = meta[0].astype(jnp.int32)
    slot = meta[1].astype(jnp.int32)
    plane = expert // (2 * ROW)
    row = (expert & (2 * ROW - 1)) * capacity + slot
    span = 2 * ROW * capacity
    first = lax.rem(z + 1 + c * (planes - 2), planes)
    second = lax.rem(z + 2 + c * (planes - 4), planes)
    return jnp.where(plane == first, row, jnp.where(plane == second, row + span, -1))


def compact_rows(capacity, b, rows, index):
    _, x, c = place()
    local = sum((index >= m * capacity).astype(jnp.int32) for m in range(1, 2 * ROW))
    return piece_of(local, x, c) * rows + b * capacity + index - local * capacity


def one_hot(rows, total):
    lines = iota((total, rows.shape[1]), 0)
    return sum((lines == rows[k : k + 1]).astype(F32) for k in range(rows.shape[0]))


def weighted(rows, gates, total):
    lines = iota((total, rows.shape[1]), 0)
    return sum(jnp.where(lines == rows[k : k + 1], gates[k : k + 1], 0.0) for k in range(TOPK))


def gather_body(capacity, kinds, rows, *refs):
    outs, refs = refs[-ROW:], refs[:-ROW]
    total = 2 * ROW * rows
    span = 2 * ROW * capacity
    picks, values = [], []
    for b, (meta, at, block) in enumerate(kinds):
        if meta is not None:
            picks.append(one_hot(dense_rows(refs[meta], b, capacity, rows), total))
            values.append(refs[block][...])
        else:
            picks.append(one_hot(compact_rows(capacity, b, rows, iota((1, span), 1)), total))
            values.append(refs[block][at : at + span])
    got = jnp.dot(
        jnp.concatenate(picks, axis=1).astype(BF16), jnp.concatenate(values, axis=0), preferred_element_type=F32
    ).astype(BF16)
    for s in range(ROW):
        for o in range(2):
            at = (s * 2 + o) * rows
            outs[s][o] = got[at : at + rows]


def far_body(planes, capacity, meta, block, out):
    pick = one_hot(far_rows(meta, planes, capacity), out.shape[0]).astype(BF16)
    out[...] = jnp.dot(pick, block[...], preferred_element_type=F32).astype(BF16)


def expert_body(x0, x1, x2, x3, gain, g0, u0, d0, g1, u1, d1, y0, y1, y2, y3):
    xs, ys = (x0, x1, x2, x3), (y0, y1, y2, y3)
    rows = x0.shape[1]
    for o, (g, u, d) in enumerate(((g0, u0, d0), (g1, u1, d1))):
        values = jnp.concatenate([v[o].astype(F32) for v in xs], axis=0)
        normed = normalized(values, gain[...])
        gate = jnp.dot(normed, g[...], preferred_element_type=F32)
        upper = jnp.dot(normed, u[...], preferred_element_type=F32)
        hidden = (silu(gate) * upper).astype(BF16)
        out = jnp.dot(hidden, d[...], preferred_element_type=F32).astype(BF16)
        for s in range(ROW):
            ys[s][o] = out[s * rows : (s + 1) * rows]


def transposed_dot(a, b):
    return lax.dot_general(a, b, (((0,), (0,)), ((), ())), preferred_element_type=F32)


def rows_body(capacity, count, r0, r1, r2, r3, *outs):
    rows = r0.shape[1]
    total = 2 * ROW * rows
    results = jnp.concatenate([r[o] for r in (r0, r1, r2, r3) for o in range(2)], axis=0)
    for b in range(count):
        span = outs[b].shape[0]
        target = compact_rows(capacity, b, rows, iota((span, total), 0))
        pick = (iota((span, total), 1) == target).astype(BF16)
        outs[b][...] = jnp.dot(pick, results, preferred_element_type=F32).astype(BF16)


def share_body(capacity, picks, *refs):
    count = len(picks)
    metas, (r0, r1, r2, r3), outs = refs[:count], refs[count : count + ROW], refs[count + ROW :]
    rows = r0.shape[1]
    total = 2 * ROW * rows
    results = jnp.concatenate([r[o].astype(F32) for r in (r0, r1, r2, r3) for o in range(2)], axis=0)
    targets = [dense_rows(m, b, capacity, rows) for m, b in zip(metas, picks)]
    gates = sum(jnp.sum(weighted(t, m[2], total), axis=1, keepdims=True) for t, m in zip(targets, metas))
    scaled = (results * gates).astype(BF16)
    for n in range(count):
        pick = one_hot(targets[n], total).astype(BF16)
        outs[n][...] = transposed_dot(pick, scaled).astype(BF16)


def add_body(planes, capacity, meta, share, far, out):
    target = far_rows(meta, planes, capacity)
    total = far.shape[0]
    gates = jnp.sum(weighted(target, meta[2], total), axis=1, keepdims=True)
    scaled = (far[...].astype(F32) * gates).astype(BF16)
    pick = one_hot(target, total).astype(BF16)
    out[...] = (share[...].astype(F32) + transposed_dot(pick, scaled)).astype(BF16)


def shared_body(own, other, gain, sg, su, sd, out_own, out_other):
    for src, dst in ((own, out_own), (other, out_other)):
        normed = normalized(src[...].astype(F32), gain[...])
        gate = jnp.dot(normed, sg[...], preferred_element_type=F32)
        upper = jnp.dot(normed, su[...], preferred_element_type=F32)
        hidden = (silu(gate) * upper).astype(BF16)
        dst[...] = jnp.dot(hidden, sd[...], preferred_element_type=F32)


def part_body(total, base, out):
    out[...] = (total[...].astype(F32) + base[...]).astype(BF16)


def norm_body(total, share, base, came, gain, kept, sent):
    value = total[...].astype(F32) + share[...].astype(F32) + base[...] + came[...].astype(F32)
    mixed = value.astype(BF16).astype(F32)
    scale = lax.rsqrt(jnp.mean(mixed * mixed, axis=1, keepdims=True) + 1e-06)
    done = (mixed * scale * gain[...]).astype(BF16)
    half = kept.shape[1]
    first = lax.axis_index("tp") == 0
    kept[...] = jnp.where(first, done[:, :half], done[:, half:])
    sent[...] = jnp.where(first, done[:, half:], done[:, :half])


def finish_body(kept, came, out):
    tokens = kept.shape[0]
    c = lax.axis_index("tp")
    out[pl.ds(pl.multiple_of(c * tokens, tokens), tokens), :] = kept[...]
    out[pl.ds(pl.multiple_of((1 - c) * tokens, tokens), tokens), :] = came[...]


def layer(tokens, expert_ids, gate_weights, norm_gain, expert_gate, expert_up, expert_down, shared_gate, shared_up, shared_down, out_gain):
    count, width = tokens.shape
    ep = lax.axis_size("ep")
    planes = ep // ROW
    experts = 2 * ep
    capacity = 3 * count * TOPK // (2 * experts)
    span = 2 * ROW * capacity
    hidden = expert_gate.shape[2]

    def ring(value, step=1):
        def to(z, c):
            return (z + (step if c == 0 else -step)) % planes

        pairs = [((z * ROW + x) * 2 + c, (to(z, c) * ROW + x) * 2 + c) for z in range(planes) for x in range(ROW) for c in range(2)]
        return lax.ppermute(value, ("ep", "tp"), pairs)

    def across(value, shift):
        if shift == 0:
            return value
        return lax.ppermute(value, "ep", [(i, i // ROW * ROW + (i + shift) % ROW) for i in range(ep)])

    def swap(value):
        return lax.ppermute(value, "tp", [(0, 1), (1, 0)])

    def shape(rows, *more, kind=BF16):
        return jax.ShapeDtypeStruct((rows, *more), kind)

    gain = norm_gain.reshape(1, width)
    (meta,) = call(functools.partial(meta_body, experts), [shape(4, TOPK, count, kind=F32)], expert_ids.T, gate_weights.T)
    known = jnp.stack([meta, swap(meta)])
    metas = {}
    for d in range(DENSE[OWN] + 1):
        if d:
            known = ring(known)
        metas[OWN, d], metas[OTHER, d] = known[0], known[1]
    blocks = {(OWN, 0): tokens, (OTHER, 0): swap(tokens)}
    for b in (OWN, OTHER):
        for d in range(1, DENSE[b] + 1):
            blocks[b, d] = ring(blocks[b, d - 1])
        d = DENSE[b]
        (far,) = call(functools.partial(far_body, planes, capacity), [shape(2 * span, width)], metas[b, d], blocks[b, d], flops=4 * span * count * width)
        blocks[b, d + 1] = ring(far)
        blocks[b, d + 2] = ring(blocks[b, d + 1][span:])
    weights = [w[0] for w in (expert_gate, expert_up, expert_down)]
    weights += [swap(w) for w in weights]

    back = []
    for batch in BATCHES:
        n = len(batch)
        rows = -(-n * capacity // 8) * 8
        args, kinds = [], []
        for b, d in batch:
            if d <= DENSE[b]:
                kinds.append((len(args), None, len(args) + 1))
                args += [metas[b, d], blocks[b, d]]
            else:
                kinds.append((None, 0, len(args)))
                args.append(blocks[b, d])
        piece = [shape(2, rows, width)] * ROW
        flops = sum(4 * ROW * rows * count * width for _ in batch)
        sent = call(functools.partial(gather_body, capacity, kinds, rows), piece, *args, flops=flops, limit=20)
        came = [across(v, s) for s, v in enumerate(sent)]
        made = call(expert_body, piece, *came, gain, *weights, flops=12 * ROW * rows * width * hidden, limit=20)
        back.append([across(v, -s) for s, v in enumerate(made)])

    shares = {}
    for a, places in ((1, (3, 2, 1, 0)), (0, (7, 6, 5, 4)), (0, (3, 2, 1, 0))):
        keys = [BATCHES[a][i] for i in places]
        got = call(
            functools.partial(share_body, capacity, places), [shape(count, width)] * len(keys),
            *[metas[k] for k in keys], *back[a], flops=len(keys) * 4 * ROW * back[a][0].shape[1] * count * width, limit=20,
        )
        shares.update(zip(keys, got))
    compact = call(functools.partial(rows_body, capacity, len(BATCHES[2])), [shape(span, width)] * len(BATCHES[2]), *back[2], flops=8 * ROW * span * span * width)
    compact = dict(zip(BATCHES[2], compact))
    totals = {}
    for b in (OWN, OTHER):
        d = DENSE[b]
        came = ring(compact[b, d + 2], -1)
        came = ring(jnp.concatenate([compact[b, d + 1], came]), -1)
        (total,) = call(functools.partial(add_body, planes, capacity), [shape(count, width)], metas[b, d], shares[b, d], came, flops=4 * span * count * width)
        for d in range(DENSE[b], 0, -1):
            if d < DENSE[b]:
                total = (total.astype(F32) + shares[b, d].astype(F32)).astype(BF16)
            total = ring(total, -1)
        totals[b] = total

    base = call(
        shared_body, [shape(count, width, kind=F32)] * 2, tokens, blocks[OTHER, 0], gain, shared_gate, shared_up, shared_down,
        flops=12 * count * width * shared_gate.shape[1],
    )
    (part,) = call(part_body, [shape(count, width)], totals[OTHER], base[1])
    half = width // 2
    kept, sent = call(
        norm_body, [shape(count, half)] * 2, totals[OWN], shares[OWN, 0], base[0], swap(part), out_gain.reshape(1, width)
    )
    (out,) = call(finish_body, [shape(2 * count, half)], kept, swap(sent))
    return out


def solution(mesh):
    in_specs = (
        P(("grp", "ep", "tp"), None),
        P(("grp", "ep", "tp"), None),
        P(("grp", "ep", "tp"), None),
        P(),
        P(("ep", "tp"), None, None),
        P(("ep", "tp"), None, None),
        P(("ep", "tp"), None, None),
        P(None, "tp"),
        P(None, "tp"),
        P("tp", None),
        P(),
    )
    out_specs = P(("grp", "ep"), "tp")
    return jax.shard_map(layer, mesh=mesh, in_specs=in_specs, out_specs=out_specs, check_vma=False)
```

```python
import functools

import jax
import jax.numpy as jnp
from jax import lax
from jax.experimental import pallas as pl
from jax.experimental.pallas import tpu as pltpu
from jax.sharding import PartitionSpec as P


TOPK = 4
ROW = 4
SPACE = 14
F32 = jnp.float32
BF16 = jnp.bfloat16
VMEM = pl.BlockSpec(memory_space=pltpu.VMEM)
OWN, OTHER = "own", "other"
BATCHES = (
    ((OWN, 0), (OWN, 1), (OTHER, 1), (OWN, 2), (OTHER, 2)),
    ((OWN, 3), (OTHER, 3), (OWN, 4)),
    ((OTHER, 4), (OWN, 5), (OTHER, 5), (OTHER, 6)),
    ((OWN, 6), (OWN, 7), (OTHER, 7), (OWN, 8)),
)
DENSE = {OWN: 6, OTHER: 5}


def iota(shape, dim):
    return lax.broadcasted_iota(jnp.int32, shape, dim)


def call(body, outs, *args, flops=0, limit=12):
    moved = sum(a.size * a.dtype.itemsize for a in (*args, *outs))
    return pl.pallas_call(
        body,
        out_shape=tuple(outs),
        in_specs=[VMEM] * len(args),
        out_specs=tuple(VMEM for _ in outs),
        compiler_params=pltpu.CompilerParams(vmem_limit_bytes=limit << 20),
        cost_estimate=pl.CostEstimate(flops=flops, bytes_accessed=moved, transcendentals=0),
    )(*args)


def place():
    ep = lax.axis_index("ep")
    return ep // ROW, ep % ROW, lax.axis_index("tp")


def normalized(values, gain):
    scale = lax.rsqrt(jnp.mean(values * values, axis=1, keepdims=True) + 1e-06)
    return (values * scale * gain).astype(BF16)


def silu(v):
    return v / (1.0 + jnp.exp(-v))


def meta_body(experts, ids_ref, gates_ref, out_ref):
    tokens = ids_ref.shape[1]
    ids = ids_ref[...]
    named = [(iota((experts, tokens), 0) == ids[k : k + 1]).astype(F32) for k in range(TOPK)]
    before = (iota((tokens, tokens), 0) < iota((tokens, tokens), 1)).astype(BF16)
    count = jnp.dot(sum(named).astype(BF16), before, preferred_element_type=F32)
    out_ref[0] = ids.astype(F32)
    for k in range(TOPK):
        out_ref[1, k : k + 1] = jnp.sum(named[k] * count, axis=0, keepdims=True)
    out_ref[2] = gates_ref[...]
    out_ref[3] = jnp.zeros_like(gates_ref)


def spacer_body(passes, meta, out, work):
    out[...] = meta[...]

    @pl.when(jnp.max(meta[...]) < -1.0)
    def _():
        value = work[...] + jnp.sum(meta[...])
        for _ in range(passes):
            value = silu(value)
        out[...] = out[...] + jnp.sum(value)


def piece_of(local, x, c):
    shift = ((local >> 1) - x) & (ROW - 1)
    return shift * 2 + ((local & 1) ^ c)


def dense_rows(meta, b, capacity, rows):
    z, x, c = place()
    expert = meta[0].astype(jnp.int32)
    slot = meta[1].astype(jnp.int32)
    row = piece_of(expert & (2 * ROW - 1), x, c) * rows + b * capacity + slot
    return jnp.where((expert // (2 * ROW)) == z, row, -1)


def far_rows(meta, planes, capacity):
    z, _, c = place()
    expert = meta[0].astype(jnp.int32)
    slot = meta[1].astype(jnp.int32)
    plane = expert // (2 * ROW)
    row = (expert & (2 * ROW - 1)) * capacity + slot
    span = 2 * ROW * capacity
    first = lax.rem(z + 1 + c * (planes - 2), planes)
    second = lax.rem(z + 2 + c * (planes - 4), planes)
    return jnp.where(plane == first, row, jnp.where(plane == second, row + span, -1))


def compact_rows(capacity, b, rows, index):
    _, x, c = place()
    local = sum((index >= m * capacity).astype(jnp.int32) for m in range(1, 2 * ROW))
    return piece_of(local, x, c) * rows + b * capacity + index - local * capacity


def one_hot(rows, total):
    lines = iota((total, rows.shape[1]), 0)
    return sum((lines == rows[k : k + 1]).astype(F32) for k in range(rows.shape[0]))


def weighted(rows, gates, total):
    lines = iota((total, rows.shape[1]), 0)
    return sum(jnp.where(lines == rows[k : k + 1], gates[k : k + 1], 0.0) for k in range(TOPK))


def gather_body(capacity, kinds, rows, *refs):
    outs, refs = refs[-ROW:], refs[:-ROW]
    total = 2 * ROW * rows
    span = 2 * ROW * capacity
    picks, values = [], []
    for b, (meta, at, block) in enumerate(kinds):
        if meta is not None:
            picks.append(one_hot(dense_rows(refs[meta], b, capacity, rows), total))
            values.append(refs[block][...])
        else:
            picks.append(one_hot(compact_rows(capacity, b, rows, iota((1, span), 1)), total))
            values.append(refs[block][at : at + span])
    got = jnp.dot(
        jnp.concatenate(picks, axis=1).astype(BF16), jnp.concatenate(values, axis=0), preferred_element_type=F32
    ).astype(BF16)
    for s in range(ROW):
        for o in range(2):
            at = (s * 2 + o) * rows
            outs[s][o] = got[at : at + rows]


def far_body(planes, capacity, meta, block, near, far):
    span = near.shape[0]
    pick = one_hot(far_rows(meta, planes, capacity), 2 * span).astype(BF16)
    got = jnp.dot(pick, block[...], preferred_element_type=F32).astype(BF16)
    near[...] = got[:span]
    far[...] = got[span:]


def expert_body(x0, x1, x2, x3, gain, g0, u0, d0, g1, u1, d1, y0, y1, y2, y3):
    xs, ys = (x0, x1, x2, x3), (y0, y1, y2, y3)
    rows = x0.shape[1]
    for o, (g, u, d) in enumerate(((g0, u0, d0), (g1, u1, d1))):
        values = jnp.concatenate([v[o].astype(F32) for v in xs], axis=0)
        normed = normalized(values, gain[...])
        gate = jnp.dot(normed, g[...], preferred_element_type=F32)
        upper = jnp.dot(normed, u[...], preferred_element_type=F32)
        hidden = (silu(gate) * upper).astype(BF16)
        out = jnp.dot(hidden, d[...], preferred_element_type=F32).astype(BF16)
        for s in range(ROW):
            ys[s][o] = out[s * rows : (s + 1) * rows]


def transposed_dot(a, b):
    return lax.dot_general(a, b, (((0,), (0,)), ((), ())), preferred_element_type=F32)


def rows_body(capacity, places, r0, r1, r2, r3, *outs):
    rows = r0.shape[1]
    total = 2 * ROW * rows
    results = jnp.concatenate([r[o] for r in (r0, r1, r2, r3) for o in range(2)], axis=0)
    for b, out in zip(places, outs):
        span = out.shape[0]
        target = compact_rows(capacity, b, rows, iota((span, total), 0))
        pick = (iota((span, total), 1) == target).astype(BF16)
        out[...] = jnp.dot(pick, results, preferred_element_type=F32).astype(BF16)


def share_body(capacity, picks, *refs):
    count = len(picks)
    metas, (r0, r1, r2, r3), outs = refs[:count], refs[count : count + ROW], refs[count + ROW :]
    rows = r0.shape[1]
    total = 2 * ROW * rows
    results = jnp.concatenate([r[o].astype(F32) for r in (r0, r1, r2, r3) for o in range(2)], axis=0)
    targets = [dense_rows(m, b, capacity, rows) for m, b in zip(metas, picks)]
    gates = sum(jnp.sum(weighted(t, m[2], total), axis=1, keepdims=True) for t, m in zip(targets, metas))
    scaled = (results * gates).astype(BF16)
    for n in range(count):
        pick = one_hot(targets[n], total).astype(BF16)
        outs[n][...] = transposed_dot(pick, scaled).astype(BF16)


def add_body(planes, capacity, meta, share, near, far, out):
    target = far_rows(meta, planes, capacity)
    total = 2 * near.shape[0]
    gates = jnp.sum(weighted(target, meta[2], total), axis=1, keepdims=True)
    rows = jnp.concatenate([near[...].astype(F32), far[...].astype(F32)], axis=0)
    pick = one_hot(target, total).astype(BF16)
    out[...] = (share[...].astype(F32) + transposed_dot(pick, (rows * gates).astype(BF16))).astype(BF16)


def shared_body(own, other, gain, sg, su, sd, out_own, out_other):
    for src, dst in ((own, out_own), (other, out_other)):
        normed = normalized(src[...].astype(F32), gain[...])
        gate = jnp.dot(normed, sg[...], preferred_element_type=F32)
        upper = jnp.dot(normed, su[...], preferred_element_type=F32)
        hidden = (silu(gate) * upper).astype(BF16)
        dst[...] = jnp.dot(hidden, sd[...], preferred_element_type=F32)


def norm_body(own, other, share, base, came, gain, kept, sent):
    value = own[...].astype(F32) + other[...].astype(F32) + share[...].astype(F32) + base[...] + came[...]
    mixed = value.astype(BF16).astype(F32)
    scale = lax.rsqrt(jnp.mean(mixed * mixed, axis=1, keepdims=True) + 1e-06)
    done = (mixed * scale * gain[...]).astype(BF16)
    half = kept.shape[1]
    first = lax.axis_index("tp") == 0
    kept[...] = jnp.where(first, done[:, :half], done[:, half:])
    sent[...] = jnp.where(first, done[:, half:], done[:, :half])


def finish_body(kept, came, out):
    tokens = kept.shape[0]
    c = lax.axis_index("tp")
    out[pl.ds(pl.multiple_of(c * tokens, tokens), tokens), :] = kept[...]
    out[pl.ds(pl.multiple_of((1 - c) * tokens, tokens), tokens), :] = came[...]


def layer(tokens, expert_ids, gate_weights, norm_gain, expert_gate, expert_up, expert_down, shared_gate, shared_up, shared_down, out_gain):
    count, width = tokens.shape
    ep = lax.axis_size("ep")
    planes = ep // ROW
    experts = 2 * ep
    capacity = 3 * count * TOPK // (2 * experts)
    span = 2 * ROW * capacity
    hidden = expert_gate.shape[2]

    def ring(value, step=1, flip=0):
        def to(z, c):
            return (z + (step if c == 0 else -step)) % planes

        pairs = [((z * ROW + x) * 2 + c, (to(z, c) * ROW + x) * 2 + (c ^ flip)) for z in range(planes) for x in range(ROW) for c in range(2)]
        return lax.ppermute(value, ("ep", "tp"), pairs)

    def across(value, shift):
        if shift == 0:
            return value
        return lax.ppermute(value, "ep", [(i, i // ROW * ROW + (i + shift) % ROW) for i in range(ep)])

    def swap(value):
        return lax.ppermute(value, "tp", [(0, 1), (1, 0)])

    def shape(rows, *more, kind=BF16):
        return jax.ShapeDtypeStruct((rows, *more), kind)

    gain = norm_gain.reshape(1, width)
    (meta,) = call(functools.partial(meta_body, experts), [shape(4, TOPK, count, kind=F32)], expert_ids.T, gate_weights.T)
    known = jnp.stack([meta, swap(meta)])
    first = pl.pallas_call(
        functools.partial(spacer_body, SPACE),
        out_shape=jax.ShapeDtypeStruct(known.shape, F32),
        in_specs=[VMEM],
        out_specs=VMEM,
        scratch_shapes=[pltpu.VMEM((512, 1024), F32)],
        compiler_params=pltpu.CompilerParams(vmem_limit_bytes=12 << 20),
        name="spacer",
    )
    first = first(known)
    metas = {}
    for d in range(DENSE[OWN] + 1):
        if d:
            known = ring(known)
        metas[OWN, d], metas[OTHER, d] = (known if d else first)[0], (known if d else first)[1]
    blocks = {(OWN, 0): tokens, (OTHER, 0): swap(tokens)}
    for b in (OWN, OTHER):
        for d in range(1, DENSE[b] + 1):
            blocks[b, d] = ring(blocks[b, d - 1])
        d = DENSE[b]
        near, far = call(
            functools.partial(far_body, planes, capacity), [shape(span, width)] * 2, metas[b, d], blocks[b, d],
            flops=4 * span * count * width,
        )
        blocks[b, d + 1] = ring(near)
        blocks[b, d + 2] = ring(far, 2)
    weights = [w[0] for w in (expert_gate, expert_up, expert_down)]
    weights += [swap(w) for w in weights]

    back = []
    for batch in BATCHES:
        n = len(batch)
        rows = -(-n * capacity // 8) * 8
        args, kinds = [], []
        for b, d in batch:
            if d <= DENSE[b]:
                kinds.append((len(args), None, len(args) + 1))
                args += [metas[b, d], blocks[b, d]]
            else:
                kinds.append((None, 0, len(args)))
                args.append(blocks[b, d])
        piece = [shape(2, rows, width)] * ROW
        flops = sum(4 * ROW * rows * count * width for _ in batch)
        sent = call(functools.partial(gather_body, capacity, kinds, rows), piece, *args, flops=flops, limit=20)
        came = [across(v, s) for s, v in enumerate(sent)]
        made = call(expert_body, piece, *came, gain, *weights, flops=12 * ROW * rows * width * hidden, limit=20)
        back.append([across(v, -s) for s, v in enumerate(made)])

    shares = {}
    for a, places in ((3, (0,)), (2, (2, 1, 0)), (1, (2, 1, 0)), (0, (4, 3, 2, 1, 0))):
        keys = [BATCHES[a][i] for i in places]
        got = call(
            functools.partial(share_body, capacity, places), [shape(count, width)] * len(keys),
            *[metas[k] for k in keys], *back[a], flops=len(keys) * 4 * ROW * back[a][0].shape[1] * count * width, limit=20,
        )
        shares.update(zip(keys, got))
    compact = {}
    for a, places in ((3, (3, 2, 1)), (2, (3,))):
        keys = [BATCHES[a][i] for i in places]
        got = call(
            functools.partial(rows_body, capacity, places), [shape(span, width)] * len(keys), *back[a],
            flops=len(keys) * 4 * ROW * back[a][0].shape[1] * span * width,
        )
        compact.update(zip(keys, got))
    totals = {}
    for b in (OWN, OTHER):
        d = DENSE[b]
        far = ring(compact[b, d + 2], -2)
        near = ring(compact[b, d + 1], -1)
        (total,) = call(
            functools.partial(add_body, planes, capacity), [shape(count, width)], metas[b, d], shares[b, d], near, far,
            flops=4 * span * count * width,
        )
        for d in range(DENSE[b], 0, -1):
            if d < DENSE[b]:
                total = (total.astype(F32) + shares[b, d].astype(F32)).astype(BF16)
            total = ring(total, -1, int(b == OTHER and d == 1))
        totals[b] = total

    base = call(
        shared_body, [shape(count, width, kind=F32)] * 2, tokens, blocks[OTHER, 0], gain, shared_gate, shared_up, shared_down,
        flops=12 * count * width * shared_gate.shape[1],
    )
    half = width // 2
    kept, sent = call(
        norm_body, [shape(count, half)] * 2, totals[OWN], totals[OTHER], shares[OWN, 0], base[0], swap(base[1]),
        out_gain.reshape(1, width),
    )
    (out,) = call(finish_body, [shape(2 * count, half)], kept, swap(sent))
    return out


def solution(mesh):
    in_specs = (
        P(("grp", "ep", "tp"), None),
        P(("grp", "ep", "tp"), None),
        P(("grp", "ep", "tp"), None),
        P(),
        P(("ep", "tp"), None, None),
        P(("ep", "tp"), None, None),
        P(("ep", "tp"), None, None),
        P(None, "tp"),
        P(None, "tp"),
        P("tp", None),
        P(),
    )
    out_specs = P(("grp", "ep"), "tp")
    return jax.shard_map(layer, mesh=mesh, in_specs=in_specs, out_specs=out_specs, check_vma=False)
```
